32 devices in a mesh: ep: 16 (over z, y, x), tp: 2 (over core).
Axes of the slice: x: 2, y: 2, z: 4, core: 2. Of those that a mesh axis runs over, the one named last changes fastest.
Arguments:
- stream: bfloat16 [256, 2048], P('ep', 'tp'), may hold values from -6 to 6
- hidden_state: float32 [256, 2048], P('ep', 'tp'), may hold values from -6 to 6
- conv_state: bfloat16 [256, 3, 2048], P('ep', None, 'tp'), may hold values from -6 to 6
- first_gain: float32 [2048], P('tp'), may hold values from 0.1 to 1.9
- input_weight: bfloat16 [2048, 2048], P('tp', 'ep'), may hold values from -0.125 to 0.125
- branch_weight: bfloat16 [2048, 2048], P('tp', 'ep'), may hold values from -0.125 to 0.125
- conv_taps: bfloat16 [4, 2048], P(None, 'tp'), may hold values from -3 to 3
- recur_gate: bfloat16 [32, 64, 64], P('tp'), may hold values from -0.75 to 0.75
- input_gate: bfloat16 [32, 64, 64], P('tp'), may hold values from -0.75 to 0.75
- decay_logit: float32 [2048], P('tp'), may hold values from 1.5 to 8
- output_weight: bfloat16 [2048, 2048], P('tp', 'ep'), may hold values from -0.25 to 0.25
- second_gain: float32 [2048], P('tp'), may hold values from 0.1 to 1.9
- routes: int32 [256, 2], P('ep'), may hold values from 0 to 3, all different within a row; in each aligned block of 16 rows (0 to 15, 16 to 31, ...) at most 16 rows name the same one
- route_weight: float32 [256, 2], P('ep'), may hold values from 0.25 to 1
- expert_gate: bfloat16 [2048, 12288], P(None, ('ep', 'tp')), may hold values from -0.125 to 0.125
- expert_up: bfloat16 [2048, 12288], P(None, ('ep', 'tp')), may hold values from -0.125 to 0.125
- expert_down: bfloat16 [12288, 2048], P(('ep', 'tp')), may hold values from -0.21875 to 0.21875
Outputs:
- new_stream: bfloat16 [256, 2048], P('ep', 'tp')
- new_hidden: float32 [256, 2048], P('ep', 'tp')
- new_conv: bfloat16 [256, 3, 2048], P('ep', None, 'tp')
The draws below stay inside these ranges and needn't reach their ends.
Inputs may be any that keep to these rules, and one draw needn't show every extreme that they name: `routes`: among the rows of one index of ep, no expert is named more than 16 times; in every draw some expert is named exactly 16 times by the rows of some index. Each row names different experts.
All inputs are finite; a program needn't handle non-finite values.
Results may differ from the reference program's by a relative error of at most 0.022.
Values may be sent and summed in bfloat16 or wider, within the bound.
No kernel may reach another device: no remote copies, remote signals or barrier semaphores. Data moves between devices by JAX's collectives and lax.ppermute only.
A program may use at most 128 MiB of HBM per device.

```python
import math
import jax
import jax.numpy as jnp
import numpy as np
from jax import lax

D = 2048
F = 3072
BLOCK = 64
CONV_W = 4
TOPK = 2
SEQ_DEV = 16
SEQS = 256
HEADS = 32
EXPERTS = 4
CAP = 16
N_EP = 16


def levels(key, shape, cuts, smallest, largest):
    gain = 1.0
    for axis_at, shards_of in cuts:
        draws = jax.random.uniform(jax.random.fold_in(jax.random.fold_in(key, 6), axis_at), (shards_of,), jnp.float32, smallest / len(cuts), largest / len(cuts))
        gain = gain * jnp.repeat(jnp.exp(draws), shape[axis_at] // shards_of).reshape((-1,) + (1,) * (len(shape) - 1 - axis_at))
    return gain


def assign_block(key, own, number, rows, amount, top, bound, skew):
    sequence = jax.random.permutation(key, amount)
    packed, common = load_shares(amount, rows * top, bound, skew, True), load_shares(amount, rows * top, bound, skew, False)
    places = jnp.arange(amount)

    def named(lengths, offset_by):
        used = int((lengths > 0).sum())
        fixed = max(1, used // 4)
        shifted = fixed + (places - fixed + offset_by * (used - fixed)) % max(1, amount - fixed)
        return jnp.zeros((amount,), jnp.int32).at[sequence[jnp.where(places < fixed, places, shifted)]].set(jnp.asarray(lengths, jnp.int32))

    lengths = jnp.where(number % 4 == 0, named(packed, number // 4), named(common, number - number // 4 - 1))
    mixed = jax.random.permutation(jax.random.fold_in(own, 3), amount)
    donor, sink = mixed[0:amount // 2 * 2:2], mixed[1:amount // 2 * 2:2]
    margin = jnp.minimum(lengths[donor] - 1, bound - lengths[sink]) // 2
    margin = jnp.where((donor == sequence[0]) | (sink == sequence[0]) | (lengths[sink] == 0), 0, jnp.maximum(margin, 0))
    shifted = jax.random.randint(jax.random.fold_in(own, 4), (amount // 2,), 0, 1 << 20) % (margin + 1)
    lengths = lengths.at[donor].add(-shifted).at[sink].add(shifted)
    members = jnp.searchsorted(jnp.cumsum(lengths), jnp.arange(rows * top), side="right").astype(jnp.int32)
    grid = members.reshape(top, rows).T
    grid = grid[jax.random.permutation(jax.random.fold_in(own, 1), rows)]
    offset_by = jax.random.randint(jax.random.fold_in(own, 2), (rows, 1), 0, top)
    return jnp.take_along_axis(grid, (jnp.arange(top)[None, :] + offset_by) % top, axis=1)


def load_shares(count, total, bound, skew, full):
    loads = [(1 << 20) // math.isqrt(standing ** skew) + 1 for standing in range(1, count + 1)]
    largest = bound if full else min(bound, max(-(-total // count), total * loads[0] // sum(loads)))
    least = 1 if total - largest >= count - 1 else 0
    counts, surplus = [largest] + [least] * (count - 1), total - largest - least * (count - 1)
    while surplus > 0:
        movable = [i for i in range(1, count) if counts[i] < largest] or [i for i in range(1, count) if counts[i] < bound]
        mass, remaining = sum([loads[i] for i in movable]), surplus
        for i in movable:
            more = min(bound - counts[i], max(1, remaining * loads[i] // mass), surplus)
            counts[i] = counts[i] + more
            surplus = surplus - more
    return np.array(counts)


def normal_values(own_key, shape, width, reach, cuts=(), kind=jnp.bfloat16):
    values = width * jax.random.normal(own_key, shape, jnp.float32)
    if cuts:
        values = values * levels(own_key, shape, cuts, -0.22, 0.18)
    return jnp.clip(values, -reach, reach).astype(kind)


def setup_inputs(seed: int = 0) -> dict:
    arg_keys = jax.random.split(jax.random.key(seed), 18)
    stream = normal_values(arg_keys[0], (SEQS, D), 1.0, 6.0, ((0, 16), (1, 2)))
    hidden_state = normal_values(arg_keys[1], (SEQS, D), 1.0, 6.0, ((0, 16), (1, 2)), jnp.float32)
    conv_state = normal_values(arg_keys[2], (SEQS, CONV_W - 1, D), 1.0, 6.0, ((0, 16), (2, 2)))
    first_gain = jnp.clip(1.0 + 0.18 * jax.random.normal(arg_keys[3], (D,), jnp.float32), 0.1, 1.9)
    input_weight = normal_values(arg_keys[4], (D, D), D ** -0.5, 0.125, ((0, 2), (1, 16)))
    branch_weight = normal_values(arg_keys[5], (D, D), D ** -0.5, 0.125, ((0, 2), (1, 16)))
    conv_taps = normal_values(arg_keys[6], (CONV_W, D), 0.5, 3.0, ((1, 2),))
    recur_gate = normal_values(arg_keys[7], (HEADS, BLOCK, BLOCK), BLOCK ** -0.5, 0.75, ((0, 2),))
    input_gate = normal_values(arg_keys[8], (HEADS, BLOCK, BLOCK), BLOCK ** -0.5, 0.75, ((0, 2),))
    decay_logit = jnp.clip(1.5 + 6.5 * jax.random.uniform(arg_keys[9], (D,), jnp.float32) ** levels(arg_keys[9], (D,), ((0, 2),), -0.2, 0.2), 1.5, 8.0)
    output_weight = normal_values(arg_keys[10], (D, D), (D // 4) ** -0.5, 0.25, ((0, 2), (1, 16)))
    second_gain = jnp.clip(1.0 + 0.18 * jax.random.normal(arg_keys[11], (D,), jnp.float32), 0.1, 1.9)
    routes_keys = jax.random.split(jax.random.fold_in(arg_keys[12], 1), SEQS // SEQ_DEV)
    routes_turns = jax.random.permutation(jax.random.fold_in(arg_keys[12], 3), SEQS // SEQ_DEV)
    routes = jax.vmap(lambda own, number: assign_block(jax.random.fold_in(arg_keys[12], 2), own, number, SEQ_DEV, EXPERTS, TOPK, CAP, 1))(routes_keys, routes_turns).reshape((SEQS, TOPK))
    route_weight = jnp.clip(0.25 + 0.75 * jax.random.uniform(arg_keys[13], (SEQS, TOPK), jnp.float32) ** levels(arg_keys[13], (SEQS, TOPK), ((0, 16),), -0.2, 0.2), 0.25, 1.0)
    expert_gate = normal_values(arg_keys[14], (D, EXPERTS * F), D ** -0.5, 0.125, ((1, 32),))
    expert_up = normal_values(arg_keys[15], (D, EXPERTS * F), D ** -0.5, 0.125, ((1, 32),))
    expert_down = normal_values(arg_keys[16], (EXPERTS * F, D), (F // 4) ** -0.5, 0.21875, ((0, 32),))
    return {"stream": stream, "hidden_state": hidden_state, "conv_state": conv_state, "first_gain": first_gain, "input_weight": input_weight, "branch_weight": branch_weight, "conv_taps": conv_taps, "recur_gate": recur_gate, "input_gate": input_gate, "decay_logit": decay_logit, "output_weight": output_weight, "second_gain": second_gain, "routes": routes, "route_weight": route_weight, "expert_gate": expert_gate, "expert_up": expert_up, "expert_down": expert_down}


epsilon = 1e-06
decay_power = 8.0

def block_map(values, table):
    split = values.astype(jnp.float32).reshape(SEQS, HEADS, BLOCK)
    mapped = jnp.einsum('shi,hij->shj', split, table.astype(jnp.float32))
    return mapped.reshape(SEQS, D)

def reference(stream, hidden_state, conv_state, first_gain, input_weight, branch_weight, conv_taps, recur_gate, input_gate, decay_logit, output_weight, second_gain, routes, route_weight, expert_gate, expert_up, expert_down):
    values = stream.astype(jnp.float32)
    first_power = lax.optimization_barrier(jnp.mean(values * values, axis=1, keepdims=True))
    row_scale = lax.rsqrt(first_power + epsilon)
    scaled = (values * first_gain).astype(jnp.bfloat16)
    forward = (jnp.dot(scaled, input_weight, preferred_element_type=jnp.float32) * row_scale).astype(jnp.bfloat16)
    branch = (jnp.dot(scaled, branch_weight, preferred_element_type=jnp.float32) * row_scale).astype(jnp.bfloat16)
    window = jnp.concatenate([conv_state, forward[:, None, :]], axis=1)
    new_conv = window[:, 1:]
    conv_out = jnp.einsum('skc,kc->sc', window.astype(jnp.float32), conv_taps.astype(jnp.float32)).astype(jnp.bfloat16)
    recur_open = jax.nn.sigmoid(block_map(conv_out, recur_gate))
    inward = jax.nn.sigmoid(block_map(conv_out, input_gate))
    log_decay = -decay_power * recur_open * jax.nn.softplus(-decay_logit)
    new_hidden = jnp.exp(log_decay) * hidden_state + jnp.sqrt(-jnp.expm1(2.0 * log_decay)) * (inward * conv_out.astype(jnp.float32))
    mixed = (jax.nn.gelu(branch.astype(jnp.float32)) * new_hidden).astype(jnp.bfloat16)
    middle = (values + jnp.dot(mixed, output_weight, preferred_element_type=jnp.float32)).astype(jnp.bfloat16)
    mid_values = middle.astype(jnp.float32)
    second_power = lax.optimization_barrier(jnp.mean(mid_values * mid_values, axis=1, keepdims=True))
    normed = (mid_values * lax.rsqrt(second_power + epsilon) * second_gain).astype(jnp.bfloat16)
    row_bound = CAP * N_EP

    def one_expert(carry_terms, expert_index):
        chosen = routes == expert_index
        weight = lax.optimization_barrier(jnp.sum(jnp.where(chosen, route_weight, 0.0), axis=1))
        routed = jnp.any(chosen, axis=1)
        rows = jnp.nonzero(routed, size=row_bound, fill_value=0)[0].astype(jnp.int32)
        live_rows = jnp.arange(row_bound) < jnp.sum(routed.astype(jnp.int32))
        picked = normed[rows].astype(jnp.float32)
        start = (expert_index * F).astype(jnp.int32)
        gate_cols = lax.dynamic_slice_in_dim(expert_gate, start, F, 1).astype(jnp.float32)
        up_cols = lax.dynamic_slice_in_dim(expert_up, start, F, 1).astype(jnp.float32)
        down_rows = lax.dynamic_slice_in_dim(expert_down, start, F, 0).astype(jnp.float32)
        gate_act = jnp.dot(picked, gate_cols)
        upper = jnp.dot(picked, up_cols)
        inner = lax.optimization_barrier((jax.nn.silu(gate_act) * upper).astype(jnp.bfloat16)).astype(jnp.float32)
        expert_out = jnp.dot(inner, down_rows)
        factor = jnp.where(live_rows, weight[rows], 0.0)
        return (carry_terms.at[rows].add(expert_out * factor[:, None]), None)
    expert_mix, _ = lax.scan(one_expert, jnp.zeros((SEQS, D), jnp.float32), jnp.arange(EXPERTS, dtype=jnp.int32))
    new_stream = (mid_values + expert_mix).astype(jnp.bfloat16)
    return (new_stream, new_hidden, new_conv)
```

```python
import jax
import jax.numpy as jnp
from jax import lax
from jax.sharding import PartitionSpec as P

EP_SPAN = 4
MOVE_LIMIT = 4


epsilon = 1e-06
decay_power = 8.0


def block_map(values, table):
    seq_count = values.shape[0]
    heads, inner_width, _ = table.shape
    split = values.reshape(seq_count, heads, inner_width)
    mapped = jnp.einsum("shi,hij->shj", split, table, preferred_element_type=jnp.float32)
    return mapped.reshape(seq_count, heads * inner_width)


def swap_cores(block):
    return lax.ppermute(block, "tp", [(0, 1), (1, 0)])


def own_half(block, axis):
    first, second = jnp.split(block, 2, axis=axis)
    return jnp.where(lax.axis_index("tp") == 0, first, second)


def other_half(block, axis):
    first, second = jnp.split(block, 2, axis=axis)
    return jnp.where(lax.axis_index("tp") == 0, second, first)


def plane_move(block, offset):
    count = lax.axis_size("ep")
    return lax.ppermute(block, "ep", [(i, i ^ offset) for i in range(count)])


def layer_move(block, offset):
    count = lax.axis_size("ep")
    return lax.ppermute(block, "ep", [(i, (i + offset * EP_SPAN) % count) for i in range(count)])


def layer_gather(block):
    count = lax.axis_size("ep")
    layers = count // EP_SPAN
    if layers > MOVE_LIMIT:
        groups = [[p + EP_SPAN * z for z in range(layers)] for p in range(EP_SPAN)]
        return lax.all_gather(block, "ep", axis=0, tiled=False, axis_index_groups=groups)
    own = lax.axis_index("ep") // EP_SPAN
    held = jnp.zeros((layers,) + block.shape, block.dtype)
    for offset in range(layers):
        piece = layer_move(block, offset) if offset else block
        held = lax.dynamic_update_index_in_dim(held, piece, (own - offset) % layers, 0)
    return held


def column_blocks(block, weight):
    count = lax.axis_size("ep")
    layers = count // EP_SPAN
    seq_dev = block.shape[0]
    place = lax.axis_index("ep") % EP_SPAN
    gathered = layer_gather(block).reshape(layers * seq_dev, block.shape[1])
    out = jnp.zeros((layers, EP_SPAN, seq_dev, weight.shape[1]), jnp.bfloat16)
    for offset in range(EP_SPAN):
        rows = plane_move(gathered, offset) if offset else gathered
        part = jnp.dot(rows, weight, preferred_element_type=jnp.float32).astype(jnp.bfloat16)
        part = part.reshape(layers, 1, seq_dev, weight.shape[1])
        out = lax.dynamic_update_slice(out, part, (0, place ^ offset, 0, 0))
    return out.reshape(count * seq_dev, weight.shape[1])


def whole_expert_mix(normed, routes, route_weight, expert_gate, expert_up, expert_down):
    seq_dev = normed.shape[0]
    layers = lax.axis_size("ep") // EP_SPAN
    half = own_half(normed, 1)
    half_width = half.shape[1]
    pieces = [half] + [layer_move(half, offset) for offset in range(1, layers)]
    held = jnp.concatenate(pieces, axis=0)
    plane_sum = None
    for offset in range(EP_SPAN):
        mine = plane_move(held, offset) if offset else held
        theirs = swap_cores(mine)
        first_core = lax.axis_index("tp") == 0
        rows = jnp.concatenate(
            [jnp.where(first_core, mine, theirs), jnp.where(first_core, theirs, mine)], axis=1
        )
        gate_act = jnp.dot(rows, expert_gate, preferred_element_type=jnp.float32)
        upper = jnp.dot(rows, expert_up, preferred_element_type=jnp.float32)
        inner_act = (jax.nn.silu(gate_act) * upper).astype(jnp.bfloat16)
        partial = jnp.dot(inner_act, expert_down, preferred_element_type=jnp.float32)
        arriving = swap_cores(other_half(partial, 1).astype(jnp.bfloat16))
        summed = own_half(partial, 1) + arriving.astype(jnp.float32)
        if offset:
            summed = plane_move(summed.astype(jnp.bfloat16), offset).astype(jnp.float32)
        plane_sum = summed if plane_sum is None else plane_sum + summed
    sums = plane_sum.astype(jnp.bfloat16).reshape(layers, seq_dev, half_width)
    own = lax.axis_index("ep") // EP_SPAN
    mix = jnp.zeros((seq_dev, half_width), jnp.float32)
    for offset in range(layers):
        piece = layer_move(sums[offset], -offset) if offset else sums[0]
        expert = (own + offset) % layers
        share = jnp.sum(jnp.where(routes == expert, route_weight, 0.0), axis=1, keepdims=True)
        mix = mix + share * piece.astype(jnp.float32)
    return mix


def picked_expert_mix(normed, routes, route_weight, expert_gate, expert_up, expert_down, capacity):
    seq_dev, model_width = normed.shape
    half_width = model_width // lax.axis_size("tp")
    experts = lax.axis_size("ep") // EP_SPAN
    top_count = routes.shape[1]
    flat_routes = routes.reshape(-1)
    expert_hits = (flat_routes[:, None] == jnp.arange(experts, dtype=jnp.int32)[None, :]).astype(
        jnp.int32
    )
    slot_rank = jnp.sum((jnp.cumsum(expert_hits, axis=0) - expert_hits) * expert_hits, axis=1)
    target = flat_routes * capacity + slot_rank
    picking = target[:, None] == jnp.arange(experts * capacity, dtype=jnp.int32)[None, :]
    repeated = jnp.repeat(normed, top_count, axis=0)
    buffer = jnp.einsum(
        "ae,ad->ed", picking.astype(jnp.bfloat16), repeated, preferred_element_type=jnp.float32
    ).astype(jnp.bfloat16)
    buffer = buffer.reshape(experts, capacity, normed.shape[1])
    outgoing = jnp.repeat(buffer, EP_SPAN, axis=0)
    arrived = lax.all_to_all(outgoing, "ep", split_axis=0, concat_axis=0, tiled=True)
    sources, slot_count, _ = arrived.shape
    flat_rows = arrived.reshape(sources * slot_count, model_width)
    gate_act = jnp.dot(flat_rows, expert_gate, preferred_element_type=jnp.float32)
    upper = jnp.dot(flat_rows, expert_up, preferred_element_type=jnp.float32)
    inner_act = (jax.nn.silu(gate_act) * upper).astype(jnp.bfloat16)
    partial_value = jnp.dot(inner_act, expert_down, preferred_element_type=jnp.float32)
    partial_value = lax.psum_scatter(
        partial_value.astype(jnp.bfloat16), "tp", scatter_dimension=1, tiled=True
    ).astype(jnp.float32)
    partial_value = partial_value.reshape(sources, slot_count, half_width)
    returned = lax.all_to_all(
        partial_value.astype(jnp.bfloat16), "ep", split_axis=0, concat_axis=0, tiled=True
    ).astype(partial_value.dtype)
    summed = jnp.sum(returned.reshape(experts, EP_SPAN, capacity, half_width), axis=1).reshape(
        experts * capacity, half_width
    )
    picked = jnp.dot(
        picking.astype(jnp.float32),
        summed,
        precision=lax.Precision.HIGHEST,
        preferred_element_type=jnp.float32,
    )
    expert_mix = jnp.sum(
        picked.reshape(seq_dev, top_count, half_width) * route_weight[:, :, None], axis=1
    )
    return expert_mix


def per_device(
    stream,
    hidden_state,
    conv_state,
    first_gain,
    input_weight,
    branch_weight,
    conv_taps,
    recur_gate,
    input_gate,
    decay_logit,
    output_weight,
    second_gain,
    routes,
    route_weight,
    expert_gate,
    expert_up,
    expert_down,
):
    seq_dev, half_width = stream.shape
    tp_count = lax.axis_size("tp")
    model_width = half_width * tp_count
    first_core = lax.axis_index("tp") == 0
    values = stream.astype(jnp.float32)
    scaled = (values * first_gain).astype(jnp.bfloat16)
    other_stream = swap_cores(stream)
    other_gain = swap_cores(second_gain)
    other_values = other_stream.astype(jnp.float32)
    square_sum = jnp.sum(values * values + other_values * other_values, axis=1)
    row_scale = lax.rsqrt(square_sum / model_width + epsilon)[:, None, None]
    paired = jnp.concatenate([input_weight, branch_weight], axis=1)
    partial_terms = column_blocks(scaled, paired)
    partial_terms = partial_terms.reshape(partial_terms.shape[0], 2, input_weight.shape[1])
    partial_terms = lax.all_to_all(
        partial_terms, "ep", split_axis=0, concat_axis=2, tiled=True
    )
    arriving = swap_cores(other_half(partial_terms, 2))
    partial_terms = own_half(partial_terms, 2).astype(jnp.float32) + arriving.astype(jnp.float32)
    projected = (partial_terms * row_scale).astype(jnp.bfloat16)
    forward = projected[:, 0]
    branch = projected[:, 1]
    window = jnp.concatenate([conv_state, forward[:, None, :]], axis=1)
    new_conv = window[:, 1:]
    conv_out = jnp.einsum(
        "skc,kc->sc", window.astype(jnp.float32), conv_taps.astype(jnp.float32)
    ).astype(jnp.bfloat16)
    recur_open = jax.nn.sigmoid(block_map(conv_out, recur_gate))
    inward = jax.nn.sigmoid(block_map(conv_out, input_gate))
    log_decay = -decay_power * recur_open * jax.nn.softplus(-decay_logit)
    new_hidden = jnp.exp(log_decay) * hidden_state + jnp.sqrt(-jnp.expm1(2.0 * log_decay)) * (
        inward * conv_out.astype(jnp.float32)
    )
    mixed_rows = (jax.nn.gelu(branch.astype(jnp.float32)) * new_hidden).astype(jnp.bfloat16)
    out_terms = column_blocks(mixed_rows, output_weight)
    out_terms = lax.all_to_all(out_terms, "ep", split_axis=0, concat_axis=1, tiled=True)
    out_terms = out_terms.astype(jnp.float32) + swap_cores(out_terms).astype(jnp.float32)
    full_stream = jnp.concatenate(
        [jnp.where(first_core, values, other_values), jnp.where(first_core, other_values, values)],
        axis=1,
    )
    full_gain = jnp.concatenate(
        [jnp.where(first_core, second_gain, other_gain), jnp.where(first_core, other_gain, second_gain)]
    )
    full_values = (full_stream + out_terms).astype(jnp.bfloat16).astype(jnp.float32)
    mid_values = own_half(full_values, 1)
    mean_square = jnp.mean(full_values * full_values, axis=1, keepdims=True)
    normed = (full_values * lax.rsqrt(mean_square + epsilon) * full_gain).astype(jnp.bfloat16)
    experts = lax.axis_size("ep") // EP_SPAN
    capacity = max(2, 2 * seq_dev * routes.shape[1] // experts)
    arguments = (normed, routes, route_weight, expert_gate, expert_up, expert_down)
    if capacity >= seq_dev and experts <= MOVE_LIMIT:
        expert_mix = whole_expert_mix(*arguments)
    else:
        expert_mix = picked_expert_mix(*arguments, capacity)
    new_stream = (mid_values + expert_mix).astype(jnp.bfloat16)
    return (new_stream, new_hidden, new_conv)


def solution(mesh):
    placed = (
        P("ep", "tp"),
        P("ep", "tp"),
        P("ep", None, "tp"),
        P("tp"),
        P("tp", "ep"),
        P("tp", "ep"),
        P(None, "tp"),
        P("tp", None, None),
        P("tp", None, None),
        P("tp"),
        P("tp", "ep"),
        P("tp"),
        P("ep", None),
        P("ep", None),
        P(None, ("ep", "tp")),
        P(None, ("ep", "tp")),
        P(("ep", "tp"), None),
    )
    return jax.shard_map(
        per_device,
        mesh=mesh,
        in_specs=placed,
        out_specs=(P("ep", "tp"), P("ep", "tp"), P("ep", None, "tp")),
        check_vma=False,
    )
```

```python
import jax
import jax.numpy as jnp
from jax import lax
from jax.sharding import PartitionSpec as P

EP_SPAN = 4
MOVE_LIMIT = 4


epsilon = 1e-06
decay_power = 8.0


def block_map(values, table):
    seq_count = values.shape[0]
    heads, inner_width, _ = table.shape
    split = values.reshape(seq_count, heads, inner_width)
    mapped = jnp.einsum("shi,hij->shj", split, table, preferred_element_type=jnp.float32)
    return mapped.reshape(seq_count, heads * inner_width)


def swap_cores(block):
    return lax.ppermute(block, "tp", [(0, 1), (1, 0)])


def own_half(block, axis):
    first, second = jnp.split(block, 2, axis=axis)
    return jnp.where(lax.axis_index("tp") == 0, first, second)


def other_half(block, axis):
    first, second = jnp.split(block, 2, axis=axis)
    return jnp.where(lax.axis_index("tp") == 0, second, first)


def plane_move(block, offset):
    count = lax.axis_size("ep")
    return lax.ppermute(block, "ep", [(i, i ^ offset) for i in range(count)])


def layer_move(block, offset):
    count = lax.axis_size("ep")
    return lax.ppermute(block, "ep", [(i, (i + offset * EP_SPAN) % count) for i in range(count)])


def layer_gather(block):
    count = lax.axis_size("ep")
    layers = count // EP_SPAN
    if layers > MOVE_LIMIT:
        groups = [[p + EP_SPAN * z for z in range(layers)] for p in range(EP_SPAN)]
        return lax.all_gather(block, "ep", axis=0, tiled=False, axis_index_groups=groups)
    own = lax.axis_index("ep") // EP_SPAN
    held = jnp.zeros((layers,) + block.shape, block.dtype)
    for offset in range(layers):
        piece = layer_move(block, offset) if offset else block
        held = lax.dynamic_update_index_in_dim(held, piece, (own - offset) % layers, 0)
    return held


def plane_pieces(block):
    gathered = layer_gather(block)
    return [gathered] + [plane_move(gathered, offset) for offset in range(1, EP_SPAN)]


def column_blocks(pieces, weight, gain):
    layers, seq_dev, width = pieces[0].shape
    place = lax.axis_index("ep") % EP_SPAN
    out = jnp.zeros((layers, EP_SPAN, seq_dev, weight.shape[1]), jnp.bfloat16)
    for offset, rows in enumerate(pieces):
        rows = rows.reshape(layers * seq_dev, width)
        if gain is not None:
            rows = (rows.astype(jnp.float32) * gain).astype(jnp.bfloat16)
        part = jnp.dot(rows, weight, preferred_element_type=jnp.float32).astype(jnp.bfloat16)
        part = part.reshape(layers, 1, seq_dev, weight.shape[1])
        out = lax.dynamic_update_slice(out, part, (0, place ^ offset, 0, 0))
    return out.reshape(layers * EP_SPAN * seq_dev, weight.shape[1])


def in_order(pieces):
    place = lax.axis_index("ep") % EP_SPAN
    layers, *rest = pieces[0].shape
    out = jnp.zeros((layers, EP_SPAN, *rest), pieces[0].dtype)
    for offset, piece in enumerate(pieces):
        out = lax.dynamic_update_index_in_dim(out, piece, place ^ offset, 1)
    return out


def both_halves(own, other, axis):
    first_core = lax.axis_index("tp") == 0
    return jnp.concatenate(
        [jnp.where(first_core, own, other), jnp.where(first_core, other, own)], axis=axis
    )


def whole_experts(
    stream_pieces, out_terms, full_gain, routes, route_weight, expert_gate, expert_up, expert_down
):
    layers, seq_dev, half_width = stream_pieces[0].shape
    core = lax.axis_index("tp")
    layer = lax.axis_index("ep") // EP_SPAN
    place = lax.axis_index("ep") % EP_SPAN
    all_stream = in_order(stream_pieces).reshape(-1, half_width)
    own_stream = both_halves(
        own_half(all_stream, 0), swap_cores(other_half(all_stream, 0)), 1
    ).astype(jnp.float32)
    arriving = swap_cores(other_half(out_terms, 0))
    columns = own_half(out_terms, 0).astype(jnp.float32) + arriving.astype(jnp.float32)
    columns = in_order(plane_pieces(columns.astype(jnp.bfloat16)))
    columns = columns.transpose(2, 0, 1, 3).reshape(own_stream.shape)
    middle = (own_stream + columns.astype(jnp.float32)).astype(jnp.bfloat16)
    middle = jnp.concatenate([middle, swap_cores(middle)], axis=0)
    mid_values = middle.astype(jnp.float32)
    mean_square = jnp.mean(mid_values * mid_values, axis=1, keepdims=True)
    normed = (mid_values * lax.rsqrt(mean_square + epsilon) * full_gain).astype(jnp.bfloat16)
    gate_act = jnp.dot(normed, expert_gate, preferred_element_type=jnp.float32)
    upper = jnp.dot(normed, expert_up, preferred_element_type=jnp.float32)
    inner_act = (jax.nn.silu(gate_act) * upper).astype(jnp.bfloat16)
    left_down, right_down = jnp.split(expert_down, 2, axis=1)
    left = jnp.dot(inner_act, left_down, preferred_element_type=jnp.float32).astype(jnp.bfloat16)
    right = jnp.dot(inner_act, right_down, preferred_element_type=jnp.float32).astype(jnp.bfloat16)
    arriving = swap_cores(jnp.where(core == 0, right, left))
    late, early = jnp.split(arriving, 2, axis=0)
    arriving = jnp.concatenate([early, late], axis=0).astype(jnp.float32)
    sums = jnp.where(core == 0, left, right).astype(jnp.float32) + arriving
    sums = sums.astype(jnp.bfloat16).reshape(layers, EP_SPAN, seq_dev, half_width)
    plane_sum = None
    for offset in range(EP_SPAN):
        piece = lax.dynamic_index_in_dim(sums, place ^ offset, 1, keepdims=False)
        piece = (plane_move(piece, offset) if offset else piece).astype(jnp.float32)
        plane_sum = piece if plane_sum is None else plane_sum + piece
    plane_sum = plane_sum.astype(jnp.bfloat16)
    turn = core * (layers // 2)
    mix = jnp.zeros((seq_dev, half_width), jnp.float32)
    for offset in range(layers):
        piece = lax.dynamic_index_in_dim(
            plane_sum, (layer - offset + turn) % layers, 0, keepdims=False
        )
        piece = layer_move(piece, -offset) if offset else piece
        expert = (layer + offset) % layers
        share = jnp.sum(jnp.where(routes == expert, route_weight, 0.0), axis=1, keepdims=True)
        mix = mix + share * piece.astype(jnp.float32)
    blocks = middle.reshape(layers * EP_SPAN, seq_dev, 2 * half_width)
    own_middle = lax.dynamic_index_in_dim(
        blocks, (layer + turn) % layers * EP_SPAN + place, 0, keepdims=False
    )
    return own_half(own_middle, 1).astype(jnp.float32) + mix


def picked_expert_mix(normed, routes, route_weight, expert_gate, expert_up, expert_down, capacity):
    seq_dev, model_width = normed.shape
    half_width = model_width // lax.axis_size("tp")
    experts = lax.axis_size("ep") // EP_SPAN
    top_count = routes.shape[1]
    flat_routes = routes.reshape(-1)
    expert_hits = (flat_routes[:, None] == jnp.arange(experts, dtype=jnp.int32)[None, :]).astype(
        jnp.int32
    )
    slot_rank = jnp.sum((jnp.cumsum(expert_hits, axis=0) - expert_hits) * expert_hits, axis=1)
    target = flat_routes * capacity + slot_rank
    picking = target[:, None] == jnp.arange(experts * capacity, dtype=jnp.int32)[None, :]
    repeated = jnp.repeat(normed, top_count, axis=0)
    buffer = jnp.einsum(
        "ae,ad->ed", picking.astype(jnp.bfloat16), repeated, preferred_element_type=jnp.float32
    ).astype(jnp.bfloat16)
    buffer = buffer.reshape(experts, capacity, normed.shape[1])
    outgoing = jnp.repeat(buffer, EP_SPAN, axis=0)
    arrived = lax.all_to_all(outgoing, "ep", split_axis=0, concat_axis=0, tiled=True)
    sources, slot_count, _ = arrived.shape
    flat_rows = arrived.reshape(sources * slot_count, model_width)
    gate_act = jnp.dot(flat_rows, expert_gate, preferred_element_type=jnp.float32)
    upper = jnp.dot(flat_rows, expert_up, preferred_element_type=jnp.float32)
    inner_act = (jax.nn.silu(gate_act) * upper).astype(jnp.bfloat16)
    partial_value = jnp.dot(inner_act, expert_down, preferred_element_type=jnp.float32)
    partial_value = lax.psum_scatter(
        partial_value.astype(jnp.bfloat16), "tp", scatter_dimension=1, tiled=True
    ).astype(jnp.float32)
    partial_value = partial_value.reshape(sources, slot_count, half_width)
    returned = lax.all_to_all(
        partial_value.astype(jnp.bfloat16), "ep", split_axis=0, concat_axis=0, tiled=True
    ).astype(partial_value.dtype)
    summed = jnp.sum(returned.reshape(experts, EP_SPAN, capacity, half_width), axis=1).reshape(
        experts * capacity, half_width
    )
    picked = jnp.dot(
        picking.astype(jnp.float32),
        summed,
        precision=lax.Precision.HIGHEST,
        preferred_element_type=jnp.float32,
    )
    expert_mix = jnp.sum(
        picked.reshape(seq_dev, top_count, half_width) * route_weight[:, :, None], axis=1
    )
    return expert_mix


def per_device(
    stream,
    hidden_state,
    conv_state,
    first_gain,
    input_weight,
    branch_weight,
    conv_taps,
    recur_gate,
    input_gate,
    decay_logit,
    output_weight,
    second_gain,
    routes,
    route_weight,
    expert_gate,
    expert_up,
    expert_down,
):
    seq_dev, half_width = stream.shape
    tp_count = lax.axis_size("tp")
    model_width = half_width * tp_count
    values = stream.astype(jnp.float32)
    stream_pieces = plane_pieces(stream)
    other_stream = swap_cores(stream)
    other_gain = swap_cores(second_gain)
    other_values = other_stream.astype(jnp.float32)
    square_sum = jnp.sum(values * values + other_values * other_values, axis=1)
    row_scale = lax.rsqrt(square_sum / model_width + epsilon)[:, None, None]
    paired = jnp.concatenate([input_weight, branch_weight], axis=1)
    partial_terms = column_blocks(stream_pieces, paired, first_gain)
    partial_terms = partial_terms.reshape(partial_terms.shape[0], 2, input_weight.shape[1])
    partial_terms = lax.all_to_all(
        partial_terms, "ep", split_axis=0, concat_axis=2, tiled=True
    )
    arriving = swap_cores(other_half(partial_terms, 2))
    partial_terms = own_half(partial_terms, 2).astype(jnp.float32) + arriving.astype(jnp.float32)
    projected = (partial_terms * row_scale).astype(jnp.bfloat16)
    forward = projected[:, 0]
    branch = projected[:, 1]
    window = jnp.concatenate([conv_state, forward[:, None, :]], axis=1)
    new_conv = window[:, 1:]
    conv_out = jnp.einsum(
        "skc,kc->sc", window.astype(jnp.float32), conv_taps.astype(jnp.float32)
    ).astype(jnp.bfloat16)
    recur_open = jax.nn.sigmoid(block_map(conv_out, recur_gate))
    inward = jax.nn.sigmoid(block_map(conv_out, input_gate))
    log_decay = -decay_power * recur_open * jax.nn.softplus(-decay_logit)
    new_hidden = jnp.exp(log_decay) * hidden_state + jnp.sqrt(-jnp.expm1(2.0 * log_decay)) * (
        inward * conv_out.astype(jnp.float32)
    )
    mixed_rows = (jax.nn.gelu(branch.astype(jnp.float32)) * new_hidden).astype(jnp.bfloat16)
    out_terms = column_blocks(plane_pieces(mixed_rows), output_weight, None)
    full_gain = both_halves(second_gain, other_gain, 0)
    experts = lax.axis_size("ep") // EP_SPAN
    capacity = max(2, 2 * seq_dev * routes.shape[1] // experts)
    arguments = (full_gain, routes, route_weight, expert_gate, expert_up, expert_down)
    if capacity >= seq_dev and experts <= MOVE_LIMIT and experts % 2 == 0:
        final = whole_experts(stream_pieces, out_terms, *arguments)
    else:
        out_terms = lax.all_to_all(out_terms, "ep", split_axis=0, concat_axis=1, tiled=True)
        out_terms = out_terms.astype(jnp.float32) + swap_cores(out_terms).astype(jnp.float32)
        full_values = both_halves(values, other_values, 1) + out_terms
        full_values = full_values.astype(jnp.bfloat16).astype(jnp.float32)
        mean_square = jnp.mean(full_values * full_values, axis=1, keepdims=True)
        normed = (full_values * lax.rsqrt(mean_square + epsilon) * full_gain).astype(jnp.bfloat16)
        final = own_half(full_values, 1) + picked_expert_mix(normed, *arguments[1:], capacity)
    new_stream = final.astype(jnp.bfloat16)
    return (new_stream, new_hidden, new_conv)


def solution(mesh):
    placed = (
        P("ep", "tp"),
        P("ep", "tp"),
        P("ep", None, "tp"),
        P("tp"),
        P("tp", "ep"),
        P("tp", "ep"),
        P(None, "tp"),
        P("tp", None, None),
        P("tp", None, None),
        P("tp"),
        P("tp", "ep"),
        P("tp"),
        P("ep", None),
        P("ep", None),
        P(None, ("ep", "tp")),
        P(None, ("ep", "tp")),
        P(("ep", "tp"), None),
    )
    return jax.shard_map(
        per_device,
        mesh=mesh,
        in_specs=placed,
        out_specs=(P("ep", "tp"), P("ep", "tp"), P("ep", None, "tp")),
        check_vma=False,
    )
```

```python
import jax
import jax.numpy as jnp
from jax import lax
from jax.sharding import PartitionSpec as P

EP_SPAN = 4
MOVE_LIMIT = 4


epsilon = 1e-06
decay_power = 8.0


def block_map(values, table):
    seq_count = values.shape[0]
    heads, inner_width, _ = table.shape
    split = values.reshape(seq_count, heads, inner_width)
    mapped = jnp.einsum("shi,hij->shj", split, table, preferred_element_type=jnp.float32)
    return mapped.reshape(seq_count, heads * inner_width)


def swap_cores(block):
    return lax.ppermute(block, "tp", [(0, 1), (1, 0)])


def own_half(block, axis):
    first, second = jnp.split(block, 2, axis=axis)
    return jnp.where(lax.axis_index("tp") == 0, first, second)


def other_half(block, axis):
    first, second = jnp.split(block, 2, axis=axis)
    return jnp.where(lax.axis_index("tp") == 0, second, first)


def plane_move(block, offset):
    count = lax.axis_size("ep")
    return lax.ppermute(block, "ep", [(i, i ^ offset) for i in range(count)])


def layer_move(block, offset):
    count = lax.axis_size("ep")
    return lax.ppermute(block, "ep", [(i, (i + offset * EP_SPAN) % count) for i in range(count)])


def layer_gather(block):
    count = lax.axis_size("ep")
    layers = count // EP_SPAN
    if layers > MOVE_LIMIT:
        groups = [[p + EP_SPAN * z for z in range(layers)] for p in range(EP_SPAN)]
        return lax.all_gather(block, "ep", axis=0, tiled=False, axis_index_groups=groups)
    own = lax.axis_index("ep") // EP_SPAN
    held = jnp.zeros((layers,) + block.shape, block.dtype)
    for offset in range(layers):
        piece = layer_move(block, offset) if offset else block
        held = lax.dynamic_update_index_in_dim(held, piece, (own - offset) % layers, 0)
    return held


def plane_pieces(block):
    gathered = layer_gather(block)
    return [gathered] + [plane_move(gathered, offset) for offset in range(1, EP_SPAN)]


def column_blocks(pieces, weight, gain):
    layers, seq_dev, width = pieces[0].shape
    place = lax.axis_index("ep") % EP_SPAN
    out = jnp.zeros((layers, EP_SPAN, seq_dev, weight.shape[1]), jnp.bfloat16)
    for offset, rows in enumerate(pieces):
        rows = rows.reshape(layers * seq_dev, width)
        if gain is not None:
            rows = (rows.astype(jnp.float32) * gain).astype(jnp.bfloat16)
        part = jnp.dot(rows, weight, preferred_element_type=jnp.float32).astype(jnp.bfloat16)
        part = part.reshape(layers, 1, seq_dev, weight.shape[1])
        out = lax.dynamic_update_slice(out, part, (0, place ^ offset, 0, 0))
    return out.reshape(layers * EP_SPAN * seq_dev, weight.shape[1])


def in_order(pieces):
    place = lax.axis_index("ep") % EP_SPAN
    layers, *rest = pieces[0].shape
    out = jnp.zeros((layers, EP_SPAN, *rest), pieces[0].dtype)
    for offset, piece in enumerate(pieces):
        out = lax.dynamic_update_index_in_dim(out, piece, place ^ offset, 1)
    return out


def select_order(pieces):
    place = lax.axis_index("ep") % EP_SPAN
    for bit in range((EP_SPAN - 1).bit_length()):
        turned = (place >> bit) % 2 == 1
        pieces = [
            jnp.where(turned, pieces[k ^ (1 << bit)], pieces[k]) for k in range(EP_SPAN)
        ]
    return jnp.stack(pieces, axis=1)


def both_halves(own, other, axis):
    first_core = lax.axis_index("tp") == 0
    return jnp.concatenate(
        [jnp.where(first_core, own, other), jnp.where(first_core, other, own)], axis=axis
    )


def whole_experts(
    stream_pieces, out_terms, full_gain, routes, route_weight, expert_gate, expert_up, expert_down
):
    layers, seq_dev, half_width = stream_pieces[0].shape
    core = lax.axis_index("tp")
    layer = lax.axis_index("ep") // EP_SPAN
    place = lax.axis_index("ep") % EP_SPAN
    all_stream = in_order(stream_pieces).reshape(-1, half_width)
    own_stream = both_halves(
        own_half(all_stream, 0), swap_cores(other_half(all_stream, 0)), 1
    ).astype(jnp.float32)
    arriving = swap_cores(other_half(out_terms, 0))
    columns = own_half(out_terms, 0).astype(jnp.float32) + arriving.astype(jnp.float32)
    columns = select_order(plane_pieces(columns.astype(jnp.bfloat16)))
    columns = columns.transpose(2, 0, 1, 3).reshape(own_stream.shape)
    middle = (own_stream + columns.astype(jnp.float32)).astype(jnp.bfloat16)
    middle = jnp.concatenate([middle, swap_cores(middle)], axis=0)
    mid_values = middle.astype(jnp.float32)
    mean_square = jnp.mean(mid_values * mid_values, axis=1, keepdims=True)
    normed = (mid_values * lax.rsqrt(mean_square + epsilon) * full_gain).astype(jnp.bfloat16)
    gate_act = jnp.dot(normed, expert_gate, preferred_element_type=jnp.float32)
    upper = jnp.dot(normed, expert_up, preferred_element_type=jnp.float32)
    inner_act = (jax.nn.silu(gate_act) * upper).astype(jnp.bfloat16)
    left_down, right_down = jnp.split(expert_down, 2, axis=1)
    left = jnp.dot(inner_act, left_down, preferred_element_type=jnp.float32).astype(jnp.bfloat16)
    right = jnp.dot(inner_act, right_down, preferred_element_type=jnp.float32).astype(jnp.bfloat16)
    arriving = swap_cores(jnp.where(core == 0, right, left))
    late, early = jnp.split(arriving, 2, axis=0)
    arriving = jnp.concatenate([early, late], axis=0).astype(jnp.float32)
    sums = jnp.where(core == 0, left, right).astype(jnp.float32) + arriving
    sums = sums.astype(jnp.bfloat16).reshape(layers, EP_SPAN, seq_dev, half_width)
    plane_sum = None
    for offset in range(EP_SPAN):
        piece = lax.dynamic_index_in_dim(sums, place ^ offset, 1, keepdims=False)
        piece = (plane_move(piece, offset) if offset else piece).astype(jnp.float32)
        plane_sum = piece if plane_sum is None else plane_sum + piece
    plane_sum = plane_sum.astype(jnp.bfloat16)
    turn = core * (layers // 2)
    mix = jnp.zeros((seq_dev, half_width), jnp.float32)
    for offset in range(layers):
        piece = lax.dynamic_index_in_dim(
            plane_sum, (layer - offset + turn) % layers, 0, keepdims=False
        )
        piece = layer_move(piece, -offset) if offset else piece
        expert = (layer + offset) % layers
        share = jnp.sum(jnp.where(routes == expert, route_weight, 0.0), axis=1, keepdims=True)
        mix = mix + share * piece.astype(jnp.float32)
    blocks = middle.reshape(layers * EP_SPAN, seq_dev, 2 * half_width)
    own_middle = lax.dynamic_index_in_dim(
        blocks, (layer + turn) % layers * EP_SPAN + place, 0, keepdims=False
    )
    return own_half(own_middle, 1).astype(jnp.float32) + mix


def picked_expert_mix(normed, routes, route_weight, expert_gate, expert_up, expert_down, capacity):
    seq_dev, model_width = normed.shape
    half_width = model_width // lax.axis_size("tp")
    experts = lax.axis_size("ep") // EP_SPAN
    top_count = routes.shape[1]
    flat_routes = routes.reshape(-1)
    expert_hits = (flat_routes[:, None] == jnp.arange(experts, dtype=jnp.int32)[None, :]).astype(
        jnp.int32
    )
    slot_rank = jnp.sum((jnp.cumsum(expert_hits, axis=0) - expert_hits) * expert_hits, axis=1)
    target = flat_routes * capacity + slot_rank
    picking = target[:, None] == jnp.arange(experts * capacity, dtype=jnp.int32)[None, :]
    repeated = jnp.repeat(normed, top_count, axis=0)
    buffer = jnp.einsum(
        "ae,ad->ed", picking.astype(jnp.bfloat16), repeated, preferred_element_type=jnp.float32
    ).astype(jnp.bfloat16)
    buffer = buffer.reshape(experts, capacity, normed.shape[1])
    outgoing = jnp.repeat(buffer, EP_SPAN, axis=0)
    arrived = lax.all_to_all(outgoing, "ep", split_axis=0, concat_axis=0, tiled=True)
    sources, slot_count, _ = arrived.shape
    flat_rows = arrived.reshape(sources * slot_count, model_width)
    gate_act = jnp.dot(flat_rows, expert_gate, preferred_element_type=jnp.float32)
    upper = jnp.dot(flat_rows, expert_up, preferred_element_type=jnp.float32)
    inner_act = (jax.nn.silu(gate_act) * upper).astype(jnp.bfloat16)
    partial_value = jnp.dot(inner_act, expert_down, preferred_element_type=jnp.float32)
    partial_value = lax.psum_scatter(
        partial_value.astype(jnp.bfloat16), "tp", scatter_dimension=1, tiled=True
    ).astype(jnp.float32)
    partial_value = partial_value.reshape(sources, slot_count, half_width)
    returned = lax.all_to_all(
        partial_value.astype(jnp.bfloat16), "ep", split_axis=0, concat_axis=0, tiled=True
    ).astype(partial_value.dtype)
    summed = jnp.sum(returned.reshape(experts, EP_SPAN, capacity, half_width), axis=1).reshape(
        experts * capacity, half_width
    )
    picked = jnp.dot(
        picking.astype(jnp.float32),
        summed,
        precision=lax.Precision.HIGHEST,
        preferred_element_type=jnp.float32,
    )
    expert_mix = jnp.sum(
        picked.reshape(seq_dev, top_count, half_width) * route_weight[:, :, None], axis=1
    )
    return expert_mix


def per_device(
    stream,
    hidden_state,
    conv_state,
    first_gain,
    input_weight,
    branch_weight,
    conv_taps,
    recur_gate,
    input_gate,
    decay_logit,
    output_weight,
    second_gain,
    routes,
    route_weight,
    expert_gate,
    expert_up,
    expert_down,
):
    seq_dev, half_width = stream.shape
    tp_count = lax.axis_size("tp")
    model_width = half_width * tp_count
    values = stream.astype(jnp.float32)
    stream_pieces = plane_pieces(stream)
    other_stream = swap_cores(stream)
    other_gain = swap_cores(second_gain)
    other_values = other_stream.astype(jnp.float32)
    square_sum = jnp.sum(values * values + other_values * other_values, axis=1)
    row_scale = lax.rsqrt(square_sum / model_width + epsilon)[:, None, None]
    paired = jnp.concatenate([input_weight, branch_weight], axis=1)
    partial_terms = column_blocks(stream_pieces, paired, first_gain)
    partial_terms = partial_terms.reshape(partial_terms.shape[0], 2, input_weight.shape[1])
    partial_terms = lax.all_to_all(
        partial_terms, "ep", split_axis=0, concat_axis=2, tiled=True
    )
    arriving = swap_cores(other_half(partial_terms, 2))
    partial_terms = own_half(partial_terms, 2).astype(jnp.float32) + arriving.astype(jnp.float32)
    projected = (partial_terms * row_scale).astype(jnp.bfloat16)
    forward = projected[:, 0]
    branch = projected[:, 1]
    window = jnp.concatenate([conv_state, forward[:, None, :]], axis=1)
    new_conv = window[:, 1:]
    conv_out = jnp.einsum(
        "skc,kc->sc", window.astype(jnp.float32), conv_taps.astype(jnp.float32)
    ).astype(jnp.bfloat16)
    recur_open = jax.nn.sigmoid(block_map(conv_out, recur_gate))
    inward = jax.nn.sigmoid(block_map(conv_out, input_gate))
    log_decay = -decay_power * recur_open * jax.nn.softplus(-decay_logit)
    new_hidden = jnp.exp(log_decay) * hidden_state + jnp.sqrt(-jnp.expm1(2.0 * log_decay)) * (
        inward * conv_out.astype(jnp.float32)
    )
    mixed_rows = (jax.nn.gelu(branch.astype(jnp.float32)) * new_hidden).astype(jnp.bfloat16)
    out_terms = column_blocks(plane_pieces(mixed_rows), output_weight, None)
    full_gain = both_halves(second_gain, other_gain, 0)
    experts = lax.axis_size("ep") // EP_SPAN
    capacity = max(2, 2 * seq_dev * routes.shape[1] // experts)
    arguments = (full_gain, routes, route_weight, expert_gate, expert_up, expert_down)
    if capacity >= seq_dev and experts <= MOVE_LIMIT and experts % 2 == 0:
        final = whole_experts(stream_pieces, out_terms, *arguments)
    else:
        out_terms = lax.all_to_all(out_terms, "ep", split_axis=0, concat_axis=1, tiled=True)
        out_terms = out_terms.astype(jnp.float32) + swap_cores(out_terms).astype(jnp.float32)
        full_values = both_halves(values, other_values, 1) + out_terms
        full_values = full_values.astype(jnp.bfloat16).astype(jnp.float32)
        mean_square = jnp.mean(full_values * full_values, axis=1, keepdims=True)
        normed = (full_values * lax.rsqrt(mean_square + epsilon) * full_gain).astype(jnp.bfloat16)
        final = own_half(full_values, 1) + picked_expert_mix(normed, *arguments[1:], capacity)
    new_stream = final.astype(jnp.bfloat16)
    return (new_stream, new_hidden, new_conv)


def solution(mesh):
    placed = (
        P("ep", "tp"),
        P("ep", "tp"),
        P("ep", None, "tp"),
        P("tp"),
        P("tp", "ep"),
        P("tp", "ep"),
        P(None, "tp"),
        P("tp", None, None),
        P("tp", None, None),
        P("tp"),
        P("tp", "ep"),
        P("tp"),
        P("ep", None),
        P("ep", None),
        P(None, ("ep", "tp")),
        P(None, ("ep", "tp")),
        P(("ep", "tp"), None),
    )
    return jax.shard_map(
        per_device,
        mesh=mesh,
        in_specs=placed,
        out_specs=(P("ep", "tp"), P("ep", "tp"), P("ep", None, "tp")),
        check_vma=False,
    )
```
